32 devices in a mesh: fs: 16 (over z, y, x), tp: 2 (over core).
Axes of the slice: x: 2, y: 2, z: 4, core: 2. Of those that a mesh axis runs over, the one named last changes fastest.
Arguments:
- tokens: bfloat16 [6144, 2048], P('fs', 'tp'), may hold values from -24 to 24
- mixer_gain: float32 [2048], replicated, may hold values from 0.1 to 1.9
- pool_input: bfloat16 [2048, 1024], P('fs', 'tp'), may hold values from -0.125 to 0.125
- group_weight: bfloat16 [8, 128, 128], P('tp'), may hold values from -0.5 to 0.5
- channel_scale: float32 [1024], P('tp'), may hold values from 0.5 to 2
- pool_output: bfloat16 [1024, 2048], P('tp', 'fs'), may hold values from -0.1875 to 0.1875
- ffn_gain: float32 [2048], replicated, may hold values from 0.1 to 1.9
- gate_weight: bfloat16 [2048, 5632], P('fs', 'tp'), may hold values from -0.125 to 0.125
- up_weight: bfloat16 [2048, 5632], P('fs', 'tp'), may hold values from -0.125 to 0.125
- down_weight: bfloat16 [5632, 2048], P('tp', 'fs'), may hold values from -0.078125 to 0.078125
- final_gain: float32 [2048], P('tp'), may hold values from 0.1 to 1.9
Outputs:
- normed_out: bfloat16 [6144, 2048], P('fs', 'tp')
The draws below stay inside these ranges and needn't reach their ends.
All inputs are finite; a program needn't handle non-finite values.
Results may differ from the reference program's by a relative error of at most 0.015.
Values may be sent and summed in bfloat16 or wider, within the bound.
A program may use at most 128 MiB of HBM per device.

```python
import math
import jax
import jax.numpy as jnp
from jax import lax

D = 2048
FF = 5632
GROUPS = 8
GROUP_DIM = 128
POOL = 1024
LENGTH = 128
TOKENS = 6144
N_TP = 2


def draw_tokens(key, part):
    base_key, column_key = jax.random.split(jax.random.fold_in(key, 11), 2)
    values = jax.random.normal(base_key, (TOKENS, D), jnp.float32)
    column_scales = jnp.exp(jax.random.uniform(column_key, (8,), jnp.float32, jnp.log(0.3), jnp.log(3.0)))
    values = values * jnp.repeat(column_scales, D // 8)[None, :]
    return jnp.clip(values, -24.0, 24.0).astype(jnp.bfloat16)


def level_of(rng, extent, cuts, least, high):
    level, own = 1.0, jax.random.fold_in(rng, 6)
    for axis_at, parts in cuts:
        heights = jnp.exp(jax.random.uniform(jax.random.fold_in(own, axis_at), (parts,), jnp.float32, least / len(cuts), high / len(cuts)))
        level = level * jnp.repeat(heights, extent[axis_at] // parts).reshape([-1 if axis == axis_at else 1 for axis in range(len(extent))])
    return level


def normal_values(rng, extent, scale, reach, cuts=(), kind=jnp.bfloat16):
    level = level_of(rng, extent, cuts, -0.22, 0.18) if cuts else 1.0
    array = jax.random.normal(rng, extent, jnp.float32) * scale * level
    return jnp.minimum(jnp.maximum(array, -reach), reach).astype(kind)


def setup_inputs(seed: int = 0) -> dict:
    keys = jax.random.split(jax.random.key(seed), 12)
    tokens = draw_tokens(jax.random.fold_in(keys[11], 71), 0)
    mixer_gain = jnp.clip(1.0 + 0.18 * jax.random.normal(keys[1], (D,), jnp.float32), 0.1, 1.9)
    pool_input = normal_values(keys[2], (D, POOL), D ** -0.5, 0.125, ((0, 16), (1, 2)))
    group_weight = normal_values(keys[3], (GROUPS, GROUP_DIM, GROUP_DIM), GROUP_DIM ** -0.5, 0.5, ((0, 2),))
    channel_scale = jnp.clip(jnp.exp(math.log(2.0) - 1.3862944 * jax.random.uniform(keys[4], (POOL,), jnp.float32) ** level_of(keys[4], (POOL,), ((0, 2),), -0.2, 0.2)), 0.5, 2.0)
    pool_output = normal_values(keys[5], (POOL, D), POOL ** -0.5, 0.1875, ((0, 2), (1, 16)))
    ffn_gain = jnp.clip(1.0 + 0.18 * jax.random.normal(keys[6], (D,), jnp.float32), 0.1, 1.9)
    gate_weight = normal_values(keys[7], (D, FF), D ** -0.5, 0.125, ((0, 16), (1, 2)))
    up_weight = normal_values(keys[8], (D, FF), D ** -0.5, 0.125, ((0, 16), (1, 2)))
    down_weight = normal_values(keys[9], (FF, D), FF ** -0.5, 0.078125, ((0, 2), (1, 16)))
    final_gain = jnp.clip(1.0 + 0.18 * jax.random.normal(keys[10], (D,), jnp.float32), 0.1, 1.9)
    return dict(tokens=tokens, mixer_gain=mixer_gain, pool_input=pool_input, group_weight=group_weight, channel_scale=channel_scale, pool_output=pool_output, ffn_gain=ffn_gain, gate_weight=gate_weight, up_weight=up_weight, down_weight=down_weight, final_gain=final_gain)


EPS = 1e-06

def rms(values, gain):
    wide = values.astype(jnp.float32)
    scaled = wide * jax.lax.rsqrt(lax.optimization_barrier(jnp.mean(wide * wide, axis=-1, keepdims=True)) + EPS)
    return scaled * gain.astype(jnp.float32)

def blocked_product(left, right, blocks):
    width = left.shape[1] // blocks
    total = jnp.zeros((left.shape[0], right.shape[1]), jnp.float32)
    for block in range(blocks):
        part = jnp.dot(left[:, block * width:(block + 1) * width], right[block * width:(block + 1) * width], preferred_element_type=jnp.float32)
        total = total + part.astype(jnp.bfloat16).astype(jnp.float32)
    return total

def reference(tokens, mixer_gain, pool_input, group_weight, channel_scale, pool_output, ffn_gain, gate_weight, up_weight, down_weight, final_gain):
    count_rows = tokens.shape[0]
    first_normed = rms(tokens, mixer_gain).astype(jnp.bfloat16)
    pooled_in = jnp.dot(first_normed, pool_input, preferred_element_type=jnp.float32).astype(jnp.bfloat16)
    grid = pooled_in.astype(jnp.float32).reshape(count_rows // LENGTH, LENGTH, GROUPS, GROUP_DIM)
    prefix = jnp.cumsum(grid, axis=1)
    counts = jnp.arange(1, LENGTH + 1, dtype=jnp.float32)[None, :, None]
    pieces = []
    for group in range(GROUPS):
        window = 2 ** (1 + group % 4)
        running = prefix[:, :, group]
        lagged = jnp.pad(running, ((0, 0), (window, 0), (0, 0)))[:, :LENGTH]
        average = (running - lagged) / jnp.minimum(counts, float(window))
        pieces.append(average - grid[:, :, group])
    pooled = jnp.stack(pieces, axis=2).astype(jnp.bfloat16).reshape(count_rows, GROUPS, GROUP_DIM)
    mapped = jnp.einsum('ngc,gcd->ngd', pooled.astype(jnp.float32), group_weight.astype(jnp.float32))
    grouped = (mapped.reshape(count_rows, GROUPS * GROUP_DIM) * channel_scale).astype(jnp.bfloat16)
    mixer_out = blocked_product(grouped, pool_output, N_TP)
    middle = (tokens.astype(jnp.float32) + mixer_out).astype(jnp.bfloat16)
    second_normed = rms(middle, ffn_gain).astype(jnp.bfloat16)
    gate = jnp.dot(second_normed, gate_weight, preferred_element_type=jnp.float32)
    upward = jnp.dot(second_normed, up_weight, preferred_element_type=jnp.float32)
    hidden = (jax.nn.silu(gate) * upward).astype(jnp.bfloat16)
    ffn_out = blocked_product(hidden, down_weight, N_TP)
    closing = middle.astype(jnp.float32) + ffn_out
    return rms(closing, final_gain).astype(jnp.bfloat16)
```

```python
import jax
import jax.numpy as jnp
from jax import lax
from jax.sharding import Mesh, PartitionSpec as P

GROUP_DIM = 128
LENGTH = 128
EPS = 1e-06
INNER = 4


def partner(at, step, count):
    if count & (count - 1) == 0:
        return at ^ step, at ^ step
    return (at + step) % count, (at - step) % count


def send(value, axis, count, step):
    pairs = [(at, partner(at, step, count)[0]) for at in range(count)]
    return lax.ppermute(value, axis, pairs)


def place(whole, piece, at, dim):
    return lax.dynamic_update_slice_in_dim(whole, piece, at * piece.shape[dim], dim)


def gather(value, axis, dim):
    count = lax.axis_size(axis)
    me = lax.axis_index(axis)
    shape = list(value.shape)
    shape[dim] *= count
    pieces = [(me, value)]
    for step in range(1, count):
        pieces.append((partner(me, step, count)[1], send(value, axis, count, step)))
    whole = jnp.zeros(shape, value.dtype)
    for at, piece in pieces:
        whole = place(whole, piece, at, dim)
    return whole


def exchange(value, axis, cut, dim):
    count = lax.axis_size(axis)
    me = lax.axis_index(axis)
    width = value.shape[cut] // count
    block = lambda at: lax.dynamic_slice_in_dim(value, at * width, width, cut)
    pieces = [(me, block(me))]
    for step in range(1, count):
        there, origin = partner(me, step, count)
        pieces.append((origin, send(block(there), axis, count, step)))
    shape = list(pieces[0][1].shape)
    shape[dim] *= count
    whole = jnp.zeros(shape, value.dtype)
    for at, piece in pieces:
        whole = place(whole, piece, at, dim)
    return whole


def scatter_sum(value, axis, dim):
    count = lax.axis_size(axis)
    me = lax.axis_index(axis)
    width = value.shape[dim] // count
    block = lambda at: lax.dynamic_slice_in_dim(value, at * width, width, dim)
    total = block(me).astype(jnp.float32)
    for step in range(1, count):
        there = partner(me, step, count)[0]
        total = total + send(block(there), axis, count, step).astype(jnp.float32)
    return total


def ring(value, axis, dim):
    count = lax.axis_size(axis)
    me = lax.axis_index(axis)
    shape = list(value.shape)
    shape[dim] *= count
    whole = place(jnp.zeros(shape, value.dtype), value, me, dim)
    ahead = [(at, (at + 1) % count) for at in range(count)]
    back = [(at, (at - 1) % count) for at in range(count)]
    up = down = value
    for step in range(1, count // 2 + 1):
        up = lax.ppermute(up, axis, ahead)
        whole = place(whole, up, (me - step) % count, dim)
        if 2 * step < count:
            down = lax.ppermute(down, axis, back)
            whole = place(whole, down, (me + step) % count, dim)
    return whole


def half_norm(values, gain, width):
    wide = values.astype(jnp.float32)
    squares = lax.psum(jnp.sum(wide * wide, axis=1, keepdims=True), "tp")
    return wide * lax.rsqrt(squares / width + EPS) * gain


def dot(left, right):
    return jnp.dot(left, right, preferred_element_type=jnp.float32)


def local(
    tokens,
    mixer_gain,
    pool_input,
    group_weight,
    channel_scale,
    pool_output,
    ffn_gain,
    gate_weight,
    up_weight,
    down_weight,
    final_gain,
):
    tp = lax.axis_index("tp")
    columns = tokens.shape[1]
    width = columns * lax.axis_size("tp")
    inner = lax.axis_size("inner")

    full_rows = gather(tokens, "tp", 1)
    pool_in = gather_rows(pool_input, 0)
    pool_out = gather_rows(pool_output, 1)

    hidden_width = gate_weight.shape[1] // inner
    depth = gate_weight.shape[0]
    both = jnp.concatenate(
        [
            gate_weight.reshape(depth, inner, hidden_width),
            up_weight.reshape(depth, inner, hidden_width),
        ],
        axis=2,
    ).reshape(depth, inner * 2 * hidden_width)
    both = ring(exchange(both, "inner", 1, 0), "outer", 0)
    down = ring(exchange(down_weight, "inner", 0, 1), "outer", 1)

    wide = full_rows.astype(jnp.float32)
    first_normed = (
        wide * lax.rsqrt(jnp.mean(wide * wide, axis=-1, keepdims=True) + EPS) * mixer_gain
    ).astype(jnp.bfloat16)
    row_count = first_normed.shape[0]
    pooled_in = dot(first_normed, pool_in).astype(jnp.bfloat16)
    channels = pooled_in.shape[1]
    channel_ids = tp * channels + jnp.arange(channels, dtype=jnp.int32)
    local_groups = max(group_weight.shape[0], 1)
    group_ids = tp * local_groups + jnp.arange(local_groups, dtype=jnp.int32)
    windows = jnp.left_shift(jnp.int32(2), group_ids % 4)
    later = jnp.arange(LENGTH, dtype=jnp.int32)[None, :, None]
    earlier = jnp.arange(LENGTH, dtype=jnp.int32)[None, None, :]
    reach = windows[:, None, None]
    inside = (earlier <= later) & (earlier > later - reach)
    band = inside.astype(jnp.bfloat16)
    divisor = jnp.minimum(later[:, :, 0] + 1, windows[:, None]).astype(jnp.float32)
    grid_low = pooled_in.reshape(row_count // LENGTH, LENGTH, local_groups, GROUP_DIM)
    window_sums = jnp.einsum("gts,nsgc->ntgc", band, grid_low, preferred_element_type=jnp.float32)
    average = window_sums / jnp.transpose(divisor)[None, :, :, None]
    pooled = (
        (average - grid_low.astype(jnp.float32))
        .astype(jnp.bfloat16)
        .reshape(row_count, local_groups, GROUP_DIM)
    )
    mapped = jnp.einsum("ngc,gcd->ngd", pooled, group_weight, preferred_element_type=jnp.float32)
    grouped = (mapped.reshape(row_count, local_groups * GROUP_DIM) * channel_scale).astype(
        jnp.bfloat16
    )
    mixer_terms = dot(grouped, pool_out).astype(jnp.bfloat16)
    mixer_out = scatter_sum(mixer_terms, "tp", 1)
    middle = (tokens.astype(jnp.float32) + mixer_out).astype(jnp.bfloat16)

    own_gain = lax.dynamic_slice_in_dim(ffn_gain, tp * columns, columns, 0)
    second_half = half_norm(middle, own_gain, width).astype(jnp.bfloat16)
    second_normed = gather(gather(second_half, "inner", 0), "tp", 1)
    gate = dot(second_normed, both[:, :hidden_width])
    upward = dot(second_normed, both[:, hidden_width:])
    hidden = (jax.nn.silu(gate) * upward).astype(jnp.bfloat16)
    ffn_terms = dot(hidden, down).astype(jnp.bfloat16)
    over_cores = scatter_sum(ffn_terms, "tp", 1).astype(jnp.bfloat16)
    ffn_out = scatter_sum(over_cores, "inner", 0)
    closing = middle.astype(jnp.float32) + ffn_out
    return half_norm(closing, final_gain, width).astype(jnp.bfloat16)


def gather_rows(weight, dim):
    return ring(gather(weight, "inner", dim), "outer", dim)


def solution(mesh):
    fs, tp = mesh.shape["fs"], mesh.shape["tp"]
    inner = INNER if fs % INNER == 0 else 1
    split = Mesh(mesh.devices.reshape(fs // inner, inner, tp), ("outer", "inner", "tp"))
    rows = ("outer", "inner")
    placed = (
        P(rows, "tp"),
        P(),
        P(rows, "tp"),
        P("tp", None, None),
        P("tp"),
        P("tp", rows),
        P(),
        P(rows, "tp"),
        P(rows, "tp"),
        P("tp", rows),
        P("tp"),
    )
    return jax.shard_map(
        local, mesh=split, in_specs=placed, out_specs=P(rows, "tp"), check_vma=False
    )
```

```python
import jax
import jax.numpy as jnp
from jax import lax
from jax.sharding import Mesh, PartitionSpec as P

GROUP_DIM = 128
LENGTH = 128
EPS = 1e-06
INNER = 4


def partner(at, step, count):
    if count & (count - 1) == 0:
        return at ^ step, at ^ step
    return (at + step) % count, (at - step) % count


def send(value, axis, count, step):
    pairs = [(at, partner(at, step, count)[0]) for at in range(count)]
    return lax.ppermute(value, axis, pairs)


def place(whole, piece, at, dim):
    return lax.dynamic_update_slice_in_dim(whole, piece, at * piece.shape[dim], dim)


def gather(value, axis, dim):
    count = lax.axis_size(axis)
    me = lax.axis_index(axis)
    shape = list(value.shape)
    shape[dim] *= count
    pieces = [(me, value)]
    for step in range(1, count):
        pieces.append((partner(me, step, count)[1], send(value, axis, count, step)))
    whole = jnp.zeros(shape, value.dtype)
    for at, piece in pieces:
        whole = place(whole, piece, at, dim)
    return whole


def exchange(value, axis, cut, dim):
    count = lax.axis_size(axis)
    me = lax.axis_index(axis)
    width = value.shape[cut] // count
    block = lambda at: lax.dynamic_slice_in_dim(value, at * width, width, cut)
    pieces = [(me, block(me))]
    for step in range(1, count):
        there, origin = partner(me, step, count)
        pieces.append((origin, send(block(there), axis, count, step)))
    shape = list(pieces[0][1].shape)
    shape[dim] *= count
    whole = jnp.zeros(shape, value.dtype)
    for at, piece in pieces:
        whole = place(whole, piece, at, dim)
    return whole


def scatter_sum(value, axis, dim):
    count = lax.axis_size(axis)
    me = lax.axis_index(axis)
    width = value.shape[dim] // count
    block = lambda at: lax.dynamic_slice_in_dim(value, at * width, width, dim)
    total = block(me).astype(jnp.float32)
    for step in range(1, count):
        there = partner(me, step, count)[0]
        total = total + send(block(there), axis, count, step).astype(jnp.float32)
    return total


def ring(value, axis, dim, first=None, behind=None):
    count = lax.axis_size(axis)
    me = lax.axis_index(axis)
    shape = list(value.shape)
    shape[dim] *= count
    whole = place(jnp.zeros(shape, value.dtype), value, me, dim)
    ahead = [(at, (at + 1) % count) for at in range(count)]
    back = [(at, (at - 1) % count) for at in range(count)]
    up = down = value
    for step in range(1, count // 2 + 1):
        if step == 1 and first is not None:
            up = first
        else:
            up = lax.ppermute(up, axis, ahead)
        whole = place(whole, up, (me - step) % count, dim)
        if 2 * step < count:
            if step == 1 and behind is not None:
                down = behind
            else:
                down = lax.ppermute(down, axis, back)
            whole = place(whole, down, (me + step) % count, dim)
    return whole


def half_norm(values, gain, width):
    wide = values.astype(jnp.float32)
    squares = lax.psum(jnp.sum(wide * wide, axis=1, keepdims=True), "tp")
    return wide * lax.rsqrt(squares / width + EPS) * gain


def dot(left, right):
    return jnp.dot(left, right, preferred_element_type=jnp.float32)


def local(
    tokens,
    mixer_gain,
    pool_input,
    group_weight,
    channel_scale,
    pool_output,
    ffn_gain,
    gate_weight,
    up_weight,
    down_weight,
    final_gain,
):
    tp = lax.axis_index("tp")
    columns = tokens.shape[1]
    width = columns * lax.axis_size("tp")
    inner = lax.axis_size("inner")

    full_rows = gather(tokens, "tp", 1)
    depth, hidden_all = gate_weight.shape
    hidden_width = hidden_all // inner
    both = jnp.concatenate(
        [
            gate_weight.reshape(depth, inner, hidden_width),
            up_weight.reshape(depth, inner, hidden_width),
        ],
        axis=2,
    ).reshape(depth, inner * 2 * hidden_width)
    pool_in = ring(pool_input[None, None], "outer", 0)
    pool_out = ring(pool_output[None, None], "outer", 0)
    both = exchange(both, "inner", 1, 0)
    pool_in, pool_out, both = lax.optimization_barrier((pool_in, pool_out, both))
    pool_in = gather(pool_in, "inner", 1).reshape(width, pool_input.shape[1])
    down_weight, pool_in = lax.optimization_barrier((down_weight, pool_in))
    pool_out = gather(pool_out, "inner", 1)
    pool_out = jnp.transpose(pool_out, (2, 0, 1, 3)).reshape(pool_output.shape[0], width)
    planes = lax.axis_size("outer")
    first = lax.ppermute(both, "outer", [(at, (at + 1) % planes) for at in range(planes)])
    behind = lax.ppermute(both, "outer", [(at, (at - 1) % planes) for at in range(planes)])
    down = exchange(down_weight, "inner", 0, 1)

    wide = full_rows.astype(jnp.float32)
    first_normed = (
        wide * lax.rsqrt(jnp.mean(wide * wide, axis=-1, keepdims=True) + EPS) * mixer_gain
    ).astype(jnp.bfloat16)
    row_count = first_normed.shape[0]
    pooled_in = dot(first_normed, pool_in).astype(jnp.bfloat16)
    local_groups = group_weight.shape[0]
    group_ids = tp * local_groups + jnp.arange(local_groups, dtype=jnp.int32)
    windows = jnp.left_shift(jnp.int32(2), group_ids % 4)
    later = jnp.arange(LENGTH, dtype=jnp.int32)[None, :, None]
    earlier = jnp.arange(LENGTH, dtype=jnp.int32)[None, None, :]
    reach = windows[:, None, None]
    inside = (earlier <= later) & (earlier > later - reach)
    band = inside.astype(jnp.bfloat16)
    divisor = jnp.minimum(later[:, :, 0] + 1, windows[:, None]).astype(jnp.float32)
    grid_low = pooled_in.reshape(row_count // LENGTH, LENGTH, local_groups, GROUP_DIM)
    window_sums = jnp.einsum("gts,nsgc->ntgc", band, grid_low, preferred_element_type=jnp.float32)
    average = window_sums / jnp.transpose(divisor)[None, :, :, None]
    pooled = (
        (average - grid_low.astype(jnp.float32))
        .astype(jnp.bfloat16)
        .reshape(row_count, local_groups, GROUP_DIM)
    )
    mapped = jnp.einsum("ngc,gcd->ngd", pooled, group_weight, preferred_element_type=jnp.float32)
    grouped = (mapped.reshape(row_count, local_groups * GROUP_DIM) * channel_scale).astype(
        jnp.bfloat16
    )
    mixer_terms = dot(grouped, pool_out).astype(jnp.bfloat16)
    mixer_terms, first, behind, both, down = lax.optimization_barrier(
        (mixer_terms, first, behind, both, down)
    )
    both = ring(both, "outer", 0, first, behind)
    mixer_out = scatter_sum(mixer_terms, "tp", 1)
    middle = (tokens.astype(jnp.float32) + mixer_out).astype(jnp.bfloat16)

    own_gain = lax.dynamic_slice_in_dim(ffn_gain, tp * columns, columns, 0)
    second_half = half_norm(middle, own_gain, width).astype(jnp.bfloat16)
    ahead = lax.ppermute(down, "outer", [(at, (at + 1) % planes) for at in range(planes)])
    after = lax.ppermute(down, "outer", [(at, (at - 1) % planes) for at in range(planes)])
    second_half, both, ahead, after, down = lax.optimization_barrier(
        (gather(second_half, "inner", 0), both, ahead, after, down)
    )
    down = ring(down, "outer", 1, ahead, after)
    second_normed = gather(second_half, "tp", 1)
    gate = dot(second_normed, both[:, :hidden_width])
    upward = dot(second_normed, both[:, hidden_width:])
    hidden = (jax.nn.silu(gate) * upward).astype(jnp.bfloat16)
    ffn_terms = dot(hidden, down).astype(jnp.bfloat16)
    over_cores = scatter_sum(ffn_terms, "tp", 1).astype(jnp.bfloat16)
    ffn_out = scatter_sum(over_cores, "inner", 0)
    closing = middle.astype(jnp.float32) + ffn_out
    return half_norm(closing, final_gain, width).astype(jnp.bfloat16)


def solution(mesh):
    fs, tp = mesh.shape["fs"], mesh.shape["tp"]
    inner = INNER if fs % INNER == 0 else 1
    split = Mesh(mesh.devices.reshape(fs // inner, inner, tp), ("outer", "inner", "tp"))
    rows = ("outer", "inner")
    placed = (
        P(rows, "tp"),
        P(),
        P(rows, "tp"),
        P("tp", None, None),
        P("tp"),
        P("tp", rows),
        P(),
        P(rows, "tp"),
        P(rows, "tp"),
        P("tp", rows),
        P("tp"),
    )
    return jax.shard_map(
        local, mesh=split, in_specs=placed, out_specs=P(rows, "tp"), check_vma=False
    )
```
